32 devices in a mesh: sp: 8 (over z, x), tp: 4 (over y, core).
Axes of the slice: x: 2, y: 2, z: 4, core: 2. Of those that a mesh axis runs over, the one named last changes fastest.
Arguments:
- queries: bfloat16 [4096, 512], P('sp', 'tp'), may hold values from -9.5625 to 9.5625
- keys: bfloat16 [4096, 512], P('sp', 'tp'), may hold values from -9.5625 to 9.5625
- values: bfloat16 [4096, 512], P('sp', 'tp'), may hold values from -6 to 6
- key_bias: bfloat16 [4096, 8], P('sp', 'tp'), may hold values from -17 to 0
- residual: bfloat16 [4096, 2048], P(('sp', 'tp')), may hold values from -6 to 6
- out_weight: bfloat16 [512, 2048], replicated, may hold values from -1 to 1
- norm_gain: float32 [2048], replicated, may hold values from 0.1 to 1.9
- routes: int32 [4096, 2], P(('sp', 'tp')), may hold values from 0 to 7, all different within a row; in each aligned block of 128 rows (0 to 127, 128 to 255, ...) at most 40 rows name the same one
- route_weights: float32 [4096, 2], P(('sp', 'tp')), may hold values from 0.25 to 2
- gate_weight: bfloat16 [8, 2048, 4096], P('sp', None, 'tp'), may hold values from -0.125 to 0.125
- up_weight: bfloat16 [8, 2048, 4096], P('sp', None, 'tp'), may hold values from -0.125 to 0.125
- down_weight: bfloat16 [8, 4096, 2048], P('sp', 'tp'), may hold values from -0.09375 to 0.09375
Outputs:
- output: bfloat16 [4096, 2048], P(('sp', 'tp'))
The draws below stay inside these ranges and needn't reach their ends.
Inputs may be any that keep to these rules, and one draw needn't show every extreme that they name: `routes`: each row names 2 different experts; the rows of one device name no expert more than 40 times.
All inputs are finite; a program needn't handle non-finite values.
Results may differ from the reference program's by a relative error of at most 0.017.
Values may be sent and summed in bfloat16 or wider, within the bound.
No kernel may reach another device: no remote copies, remote signals or barrier semaphores. Data moves between devices by JAX's collectives and lax.ppermute only.
A program may use at most 128 MiB of HBM per device.

```python
import math
import jax
import jax.numpy as jnp
import numpy as np
from jax import lax

D = 2048
HEAD_COUNT = 8
HEAD_DIM = 64
FF = 4096
TOP = 2
SPAN = 512
TOK_DEV = 128
TOK_SP = 512
SEQUENCE_LENGTH = 4096
EXPERTS = 8
CAP = 40
N_SP = 8
N_TP = 4


def draw_key_bias(key, part):
    gathered_keys = jax.random.split(jax.random.fold_in(key, 7), 6)
    fast_share = 0.5
    is_fast = jax.random.uniform(gathered_keys[0], (HEAD_COUNT,), jnp.float32) < fast_share
    slow_level = -jnp.log(jnp.float32(SEQUENCE_LENGTH)) - 3.0 + jax.random.uniform(gathered_keys[1], (HEAD_COUNT,), jnp.float32, minval=-0.5, maxval=0.5)
    fast_level = jax.random.uniform(gathered_keys[2], (HEAD_COUNT,), jnp.float32, minval=-7.0, maxval=-5.5)
    level = jnp.where(is_fast, fast_level, slow_level)
    block_shift = jnp.repeat(jax.random.uniform(gathered_keys[3], (N_SP,), jnp.float32, minval=-0.7, maxval=0.7), TOK_SP, total_repeat_length=SEQUENCE_LENGTH)
    sudden_position = jax.random.randint(gathered_keys[4], (4,), 0, SEQUENCE_LENGTH)
    sudden_value = jax.random.uniform(gathered_keys[5], (4, HEAD_COUNT), jnp.float32, minval=-1.5, maxval=0.0)
    position_index = jnp.arange(SEQUENCE_LENGTH, dtype=jnp.int32)
    sudden_hit_mask = (position_index[:, None] == sudden_position[None, :]).astype(jnp.float32)
    any_hit_flag = jnp.sum(sudden_hit_mask, axis=1, keepdims=True) > 0.0
    sudden_rows = jnp.dot(sudden_hit_mask, sudden_value)
    regular_rows = level[None, :] + block_shift[:, None]
    return jnp.where(any_hit_flag, sudden_rows, regular_rows).astype(jnp.bfloat16)


def levels(key, extent, pieces, smallest, high):
    factor_of = 1.0
    for position, shards_of in pieces:
        steps = jax.random.uniform(jax.random.fold_in(jax.random.fold_in(key, 6), position), (shards_of,), jnp.float32, smallest / len(pieces), high / len(pieces))
        factor_of = factor_of * jnp.repeat(jnp.exp(steps), extent[position] // shards_of).reshape((-1,) + (1,) * (len(extent) - 1 - position))
    return factor_of


def shared_out(own_key, own, number, rows, number_of, top, most, lean):
    ranking = jax.random.permutation(own_key, number_of)
    crowded, ordinary = load_shares(number_of, rows * top, most, lean, True), load_shares(number_of, rows * top, most, lean, False)
    places = jnp.arange(number_of)

    def named(lengths, offset_by):
        used = int((lengths > 0).sum())
        fixed = max(1, used // 4)
        shifted = fixed + (places - fixed + offset_by * (used - fixed)) % max(1, number_of - fixed)
        return jnp.zeros((number_of,), jnp.int32).at[ranking[jnp.where(places < fixed, places, shifted)]].set(jnp.asarray(lengths, jnp.int32))

    lengths = jnp.where(number % 4 == 0, named(crowded, number // 4), named(ordinary, number - number // 4 - 1))
    mixed = jax.random.permutation(jax.random.fold_in(own, 3), number_of)
    source_of, taker = mixed[0:number_of // 2 * 2:2], mixed[1:number_of // 2 * 2:2]
    room = jnp.minimum(lengths[source_of] - 1, most - lengths[taker]) // 2
    room = jnp.where((source_of == ranking[0]) | (taker == ranking[0]) | (lengths[taker] == 0), 0, jnp.maximum(room, 0))
    shifted = jax.random.randint(jax.random.fold_in(own, 4), (number_of // 2,), 0, 1 << 20) % (room + 1)
    lengths = lengths.at[source_of].add(-shifted).at[taker].add(shifted)
    labels = jnp.searchsorted(jnp.cumsum(lengths), jnp.arange(rows * top), side="right").astype(jnp.int32)
    table = labels.reshape(top, rows).T
    table = table[jax.random.permutation(jax.random.fold_in(own, 1), rows)]
    offset_by = jax.random.randint(jax.random.fold_in(own, 2), (rows, 1), 0, top)
    return jnp.take_along_axis(table, (jnp.arange(top)[None, :] + offset_by) % top, axis=1)


def load_shares(amount, total, reach, slope, full):
    portions = [(1 << 20) // math.isqrt(rank ** slope) + 1 for rank in range(1, amount + 1)]
    largest = reach if full else min(reach, max(-(-total // amount), total * portions[0] // sum(portions)))
    least = 1 if total - largest >= amount - 1 else 0
    given, rest = [largest] + [least] * (amount - 1), total - largest - least * (amount - 1)
    while rest > 0:
        candidates = [i for i in range(1, amount) if given[i] < largest] or [i for i in range(1, amount) if given[i] < reach]
        whole, left = sum([portions[i] for i in candidates]), rest
        for i in candidates:
            more = min(reach - given[i], max(1, left * portions[i] // whole), rest)
            given[i] = given[i] + more
            rest = rest - more
    return np.array(given)


def normal_values(rng, shape, width, bound, pieces=(), held_as=jnp.bfloat16):
    result = jax.random.normal(rng, shape, jnp.float32) * width
    if len(pieces) > 0:
        result = levels(rng, shape, pieces, -0.22, 0.18) * result
    return jnp.clip(result, min=-bound, max=bound).astype(held_as)


def setup_inputs(seed: int = 0) -> dict:
    splits = jax.random.split(jax.random.key(seed), 13)
    queries = normal_values(splits[0], (SEQUENCE_LENGTH, HEAD_COUNT * HEAD_DIM), 1.6, 9.5625, ((0, 8), (1, 4)))
    keys = normal_values(splits[1], (SEQUENCE_LENGTH, HEAD_COUNT * HEAD_DIM), 1.6, 9.5625, ((0, 8), (1, 4)))
    values = normal_values(splits[2], (SEQUENCE_LENGTH, HEAD_COUNT * HEAD_DIM), 1.0, 6.0, ((0, 8), (1, 4)))
    key_bias = draw_key_bias(jax.random.fold_in(splits[12], 71), 0)
    residual = normal_values(splits[4], (SEQUENCE_LENGTH, D), 1.0, 6.0, ((0, 32),))
    out_weight = normal_values(splits[5], (HEAD_COUNT * HEAD_DIM, D), (HEAD_COUNT * HEAD_DIM // 16) ** -0.5, 1.0)
    norm_gain = jnp.clip(1.0 + 0.18 * jax.random.normal(splits[6], (D,), jnp.float32), 0.1, 1.9)
    routes_keys = jax.random.split(jax.random.fold_in(splits[7], 1), SEQUENCE_LENGTH // TOK_DEV)
    routes_turns = jax.random.permutation(jax.random.fold_in(splits[7], 3), SEQUENCE_LENGTH // TOK_DEV)
    routes = jax.vmap(lambda own, number: shared_out(jax.random.fold_in(splits[7], 2), own, number, TOK_DEV, EXPERTS, TOP, CAP, 1))(routes_keys, routes_turns).reshape((SEQUENCE_LENGTH, TOP))
    route_weights = jnp.clip(jnp.exp(math.log(2.0) - 2.0794415 * jax.random.uniform(splits[8], (SEQUENCE_LENGTH, TOP), jnp.float32) ** levels(splits[8], (SEQUENCE_LENGTH, TOP), ((0, 32),), -0.2, 0.2)), 0.25, 2.0)
    gate_weight = normal_values(splits[9], (EXPERTS, D, FF), D ** -0.5, 0.125, ((0, 8), (2, 4)))
    up_weight = normal_values(splits[10], (EXPERTS, D, FF), D ** -0.5, 0.125, ((0, 8), (2, 4)))
    down_weight = normal_values(splits[11], (EXPERTS, FF, D), FF ** -0.5, 0.09375, ((0, 8), (1, 4)))
    return {"queries": queries, "keys": keys, "values": values, "key_bias": key_bias, "residual": residual, "out_weight": out_weight, "norm_gain": norm_gain, "routes": routes, "route_weights": route_weights, "gate_weight": gate_weight, "up_weight": up_weight, "down_weight": down_weight}


epsilon = 1e-06

def stick_span(query_block, key_block, value_block, bias_block, query_pos, key_pos):
    scores = jnp.einsum('qhd,khd->qhk', query_block, key_block) * HEAD_DIM ** (-0.5)
    scores = scores + jnp.transpose(bias_block)[None, :, :]
    earlier = key_pos[None, None, :] < query_pos[:, None, None]
    failure = jnp.where(earlier, jax.nn.log_sigmoid(-scores), 0.0)
    later_sum = lax.cumsum(failure, axis=2, reverse=True) - failure
    weights = jnp.where(earlier, jnp.exp(jax.nn.log_sigmoid(scores) + later_sum), 0.0).astype(jnp.bfloat16)
    span_out = jnp.einsum('qhk,khd->qhd', weights.astype(jnp.float32), value_block)
    return (span_out, lax.optimization_barrier(jnp.sum(failure, axis=2)))

def attend(queries, keys, values, key_bias):
    span_count = SEQUENCE_LENGTH // SPAN
    query_spans = queries.astype(jnp.float32).reshape(span_count, SPAN, HEAD_COUNT, HEAD_DIM)
    key_spans = keys.astype(jnp.float32).reshape(span_count, SPAN, HEAD_COUNT, HEAD_DIM)
    value_spans = values.astype(jnp.float32).reshape(span_count, SPAN, HEAD_COUNT, HEAD_DIM)
    bias_spans = key_bias.astype(jnp.float32).reshape(span_count, SPAN, HEAD_COUNT)

    def per_block(inputs):
        query_block, block_index = inputs
        query_pos = block_index * SPAN + jnp.arange(SPAN, dtype=jnp.int32)

        def step(held, key_index):
            running, after_total = held

            def compute():
                key_pos = key_index * SPAN + jnp.arange(SPAN, dtype=jnp.int32)
                return stick_span(query_block, key_spans[key_index], value_spans[key_index], bias_spans[key_index], query_pos, key_pos)

            def skipped():
                return (jnp.zeros((SPAN, HEAD_COUNT, HEAD_DIM), jnp.float32), jnp.zeros((SPAN, HEAD_COUNT), jnp.float32))
            span_out, span_sum = lax.cond(key_index <= block_index, compute, skipped)
            return ((running + jnp.exp(after_total)[..., None] * span_out, after_total + span_sum), None)
        start_pair = (jnp.zeros((SPAN, HEAD_COUNT, HEAD_DIM), jnp.float32), jnp.zeros((SPAN, HEAD_COUNT), jnp.float32))
        (running, _), _ = lax.scan(step, start_pair, jnp.arange(span_count, dtype=jnp.int32), reverse=True)
        return running.astype(jnp.bfloat16)
    blocks = lax.map(per_block, (query_spans, jnp.arange(span_count, dtype=jnp.int32)))
    return blocks.reshape(SEQUENCE_LENGTH, HEAD_COUNT * HEAD_DIM)

def experts_out(normed, routes, route_weights, gate_weight, up_weight, down_weight):
    most_rows = SEQUENCE_LENGTH // TOK_DEV * CAP
    flat_routes = routes.reshape(-1)
    flat_weights = route_weights.reshape(-1)
    token_of = (jnp.arange(SEQUENCE_LENGTH * TOP, dtype=jnp.int32) // TOP).astype(jnp.int32)
    block_units = FF // N_TP

    def one_expert(total, expert_index):
        chosen = flat_routes == expert_index
        picked = jnp.nonzero(chosen, size=most_rows, fill_value=0)[0].astype(jnp.int32)
        row_valid = jnp.arange(most_rows, dtype=jnp.int32) < jnp.sum(chosen.astype(jnp.int32))
        token_ids = token_of[picked]
        row_block = normed[token_ids]
        gate_act = jnp.dot(row_block, gate_weight[expert_index], preferred_element_type=jnp.float32)
        up_act = jnp.dot(row_block, up_weight[expert_index], preferred_element_type=jnp.float32)
        hidden = (jax.nn.silu(gate_act) * up_act).astype(jnp.bfloat16)
        summed = jnp.zeros((most_rows, D), jnp.float32)
        for block in range(N_TP):
            lower = block * block_units
            partial_value = jnp.dot(hidden[:, lower:lower + block_units], down_weight[expert_index, lower:lower + block_units], preferred_element_type=jnp.float32)
            summed = summed + lax.optimization_barrier(partial_value.astype(jnp.bfloat16)).astype(jnp.float32)
        expert_rows = lax.optimization_barrier(summed.astype(jnp.bfloat16)).astype(jnp.float32)
        scaled = jnp.where(row_valid[:, None], flat_weights[picked][:, None] * expert_rows, 0.0)
        return (total.at[token_ids].add(scaled), None)
    routed, _ = lax.scan(one_expert, jnp.zeros((SEQUENCE_LENGTH, D), jnp.float32), jnp.arange(EXPERTS, dtype=jnp.int32))
    return routed

def reference(queries, keys, values, key_bias, residual, out_weight, norm_gain, routes, route_weights, gate_weight, up_weight, down_weight):
    attended = attend(queries, keys, values, key_bias)
    mixed_rows = (residual.astype(jnp.float32) + jnp.dot(attended, out_weight, preferred_element_type=jnp.float32)).astype(jnp.bfloat16)
    stream = mixed_rows.astype(jnp.float32)
    normed = (stream * lax.rsqrt(lax.optimization_barrier(jnp.mean(stream * stream, axis=-1, keepdims=True)) + epsilon) * norm_gain).astype(jnp.bfloat16)
    routed = experts_out(normed, routes, route_weights, gate_weight, up_weight, down_weight)
    return (stream + routed).astype(jnp.bfloat16)
```

```python
import functools

import jax
import jax.numpy as jnp
from jax import lax
from jax.experimental import pallas as pl
from jax.experimental.pallas import tpu as pltpu
from jax.sharding import PartitionSpec as P

HEAD_DIM = 64
TOP = 2
BLOCK = 256
LANES = 128

epsilon = 1e-06


def exchange(value, axis, bit):
    return lax.ppermute(value, axis, [(i, i ^ bit) for i in range(lax.axis_size(axis))])


def split_of(sp_count):
    inner = 1
    while sp_count % (inner * 2) == 0 and (inner * 2) ** 2 <= sp_count:
        inner *= 2
    return sp_count // inner, inner


def one_block(query, key, value, bias, later_ones, acc, carry, mask):
    scores = (
        lax.dot_general(query, key, (((1,), (1,)), ((), ())), preferred_element_type=jnp.float32)
        + bias
    )
    failure = jnp.minimum(-scores, 0.0) - jnp.log(1.0 + jnp.exp(-jnp.abs(scores)))
    if mask is not None:
        failure = jnp.where(mask, failure, 0.0)
    high = failure.astype(jnp.bfloat16)
    low = (failure - high.astype(jnp.float32)).astype(jnp.bfloat16)
    later = jnp.dot(high, later_ones, preferred_element_type=jnp.float32) + jnp.dot(
        low, later_ones, preferred_element_type=jnp.float32
    )
    weights = jnp.exp((scores + failure) + (later + carry))
    if mask is not None:
        weights = jnp.where(mask, weights, 0.0)
    acc = acc + jnp.dot(weights.astype(jnp.bfloat16), value, preferred_element_type=jnp.float32)
    return acc, carry + later[:, :1] + failure[:, :1]


def head_queries(q_ref, heads):
    query = q_ref[...] * jnp.bfloat16(HEAD_DIM**-0.5)
    if heads == 1:
        return [query]
    lane_head = lax.broadcasted_iota(jnp.int32, query.shape, 1) // HEAD_DIM
    return [jnp.where(lane_head == h, query, jnp.zeros_like(query)) for h in range(heads)]


def later_matrix():
    row = lax.broadcasted_iota(jnp.int32, (BLOCK, BLOCK), 0)
    col = lax.broadcasted_iota(jnp.int32, (BLOCK, BLOCK), 1)
    return (row > col).astype(jnp.float32).astype(jnp.bfloat16)


def store_state(state, heads, acc_ref, carry_ref):
    for h in range(heads):
        acc, carry = state[h]
        acc_ref[h] = acc
        carry_ref[h] = jnp.broadcast_to(carry, carry_ref.shape[1:])


def own_kernel(q_ref, kv_ref, bias_ref, acc_ref, carry_ref, *, heads, shard_len):
    tile = pl.program_id(0)
    queries = head_queries(q_ref, heads)
    later_ones = later_matrix()
    row = lax.broadcasted_iota(jnp.int32, (BLOCK, BLOCK), 0)
    col = lax.broadcasted_iota(jnp.int32, (BLOCK, BLOCK), 1)

    def step(block, state, mask):
        key = kv_ref[pl.ds(block * BLOCK, BLOCK), :]
        value = kv_ref[pl.ds(shard_len + block * BLOCK, BLOCK), :]
        return tuple(
            one_block(
                queries[h], key, value, bias_ref[block, pl.ds(h, 1), :], later_ones, *state[h], mask
            )
            for h in range(heads)
        )

    width = q_ref.shape[1]
    empty = tuple(
        (jnp.zeros((BLOCK, width), jnp.float32), jnp.zeros((BLOCK, 1), jnp.float32))
        for _ in range(heads)
    )
    state = step(tile, empty, col < row)
    state = lax.fori_loop(0, tile, lambda i, held: step(tile - 1 - i, held, None), state)
    store_state(state, heads, acc_ref, carry_ref)


def past_kernel(
    place_ref, q_ref, kv_ref, bias_ref, acc_in, carry_in, acc_ref, carry_ref, *, heads, shard_len, inner
):
    newest, count, first, me = place_ref[0], place_ref[1], place_ref[2], place_ref[3]
    queries = head_queries(q_ref, heads)
    later_ones = later_matrix()
    blocks = shard_len // BLOCK

    def step(i, state):
        piece = newest - i // blocks
        block = blocks - 1 - i % blocks
        slot = (me // inner - piece // inner - first) * inner + (
            (piece % inner) ^ (me % inner)
        )
        key = kv_ref[slot, pl.ds(block * BLOCK, BLOCK), :]
        value = kv_ref[slot, pl.ds(shard_len + block * BLOCK, BLOCK), :]
        return tuple(
            one_block(
                queries[h],
                key,
                value,
                bias_ref[slot, block, pl.ds(h, 1), :],
                later_ones,
                *state[h],
                None,
            )
            for h in range(heads)
        )

    state = tuple((acc_in[h], carry_in[h, :, :1]) for h in range(heads))
    state = lax.fori_loop(0, count * blocks, step, state)
    store_state(state, heads, acc_ref, carry_ref)


def attend(queries, keys, values, key_bias):
    shard_len, width = queries.shape
    heads = key_bias.shape[1]
    sp_count = lax.axis_size("sp")
    outer, inner = split_of(sp_count)
    me = lax.axis_index("sp")
    blocks = shard_len // BLOCK
    tiles = shard_len // BLOCK

    bias_rows = jnp.transpose(key_bias.reshape(blocks, BLOCK, heads), (0, 2, 1)).reshape(-1, width)
    pad = -bias_rows.shape[0] % 16
    bias_count = bias_rows.shape[0]
    own = jnp.concatenate([keys, values, jnp.pad(bias_rows, ((0, pad), (0, 0)))], axis=0)

    def bias_of(pieces):
        rows = pieces[..., 2 * shard_len : 2 * shard_len + bias_count, :]
        return rows.reshape(rows.shape[:-2] + (blocks, heads, BLOCK)).astype(jnp.float32)

    columns = [own]
    for d in range(1, outer):
        columns.append(
            lax.ppermute(
                columns[-1],
                "sp",
                [(i, i + inner) for i in range(sp_count - inner)],
            )
        )
    groups = []
    for d in range(outer):
        groups.append([columns[d]] + [exchange(columns[d], "sp", k) for k in range(1, inner)])

    row_spec = pl.BlockSpec((BLOCK, width), lambda i: (i, 0))
    acc_spec = pl.BlockSpec((heads, BLOCK, width), lambda i: (0, i, 0))
    carry_spec = pl.BlockSpec((heads, BLOCK, LANES), lambda i: (0, i, 0))
    state_shape = (
        jax.ShapeDtypeStruct((heads, shard_len, width), jnp.float32),
        jax.ShapeDtypeStruct((heads, shard_len, LANES), jnp.float32),
    )
    whole = pl.BlockSpec(memory_space=pltpu.VMEM)
    state = pl.pallas_call(
        functools.partial(own_kernel, heads=heads, shard_len=shard_len),
        grid=(tiles,),
        in_specs=[row_spec, whole, whole],
        out_specs=(acc_spec, carry_spec),
        out_shape=state_shape,
        name="own_span",
    )(queries, own, bias_of(own))

    calls = [(0, min(2, outer))] + [(d, d + 1) for d in range(2, outer)]
    for first, end in calls:
        held = jnp.stack([piece for group in groups[first:end] for piece in group])
        newest = jnp.minimum(me - 1, (me // inner - first) * inner + inner - 1)
        oldest = jnp.maximum(0, (me // inner - end + 1) * inner)
        place = jnp.stack(
            [newest, jnp.maximum(newest - oldest + 1, 0), jnp.int32(first), me]
        ).astype(jnp.int32)
        state = pl.pallas_call(
            functools.partial(past_kernel, heads=heads, shard_len=shard_len, inner=inner),
            grid=(tiles,),
            in_specs=[
                pl.BlockSpec(memory_space=pltpu.SMEM),
                row_spec,
                whole,
                whole,
                acc_spec,
                carry_spec,
            ],
            out_specs=(acc_spec, carry_spec),
            out_shape=state_shape,
            name=f"past_spans_{first}",
        )(place, queries, held, bias_of(held), *state)
    acc = state[0]
    lane_head = lax.iota(jnp.int32, width)[None, :] // HEAD_DIM
    attended = acc[0]
    for h in range(1, heads):
        attended = jnp.where(lane_head == h, acc[h], attended)
    return attended.astype(jnp.bfloat16)


def shards(
    queries,
    keys,
    values,
    key_bias,
    residual,
    out_weight,
    norm_gain,
    routes,
    route_weights,
    gate_weight,
    up_weight,
    down_weight,
):
    sp_count = lax.axis_size("sp")
    tp_count = lax.axis_size("tp")
    me = lax.axis_index("sp")
    attended = attend(queries, keys, values, key_bias)
    token_heads = lax.all_to_all(attended, "tp", split_axis=0, concat_axis=1, tiled=True)
    projected = jnp.dot(token_heads, out_weight, preferred_element_type=jnp.float32)
    stream = (residual.astype(jnp.float32) + projected).astype(jnp.bfloat16).astype(jnp.float32)
    normed = (
        stream * lax.rsqrt(jnp.mean(stream * stream, axis=-1, keepdims=True) + epsilon) * norm_gain
    ).astype(jnp.bfloat16)
    token_count = residual.shape[0]
    capacity = max(2, 5 * token_count * TOP // (4 * sp_count))
    flat_routes = routes.reshape(-1)
    onehot = (flat_routes[:, None] == lax.iota(jnp.int32, sp_count)[None, :]).astype(jnp.int32)
    before = jnp.cumsum(onehot, axis=0) - onehot
    position = jnp.sum(before * onehot, axis=1).reshape(token_count, TOP)
    place = routes ^ me

    first = min(capacity, -(-capacity // 16) * 8)
    chunks = [(0, first)] + ([(first, capacity)] if first < capacity else [])

    bits = []
    bit = 1
    while bit < tp_count:
        bits.append(bit)
        bit *= 2

    sent = []
    combine = []
    for begin, end in chunks:
        rows = end - begin
        inside = (position >= begin) & (position < end)
        slot = jnp.where(inside, place * rows + position - begin, -1)
        select = slot[:, :, None] == lax.iota(jnp.int32, sp_count * rows)[None, None, :]
        placing = jnp.any(select, axis=1).astype(jnp.bfloat16)
        combine.append(jnp.sum(jnp.where(select, route_weights[:, :, None], 0.0), axis=1))
        outgoing = jnp.einsum(
            "ts,td->sd", placing, normed, preferred_element_type=jnp.float32
        ).astype(jnp.bfloat16)
        sent.append(outgoing)

    routed = None
    for (begin, end), outgoing, weight in zip(chunks, sent, combine):
        rows = end - begin
        arrived = jnp.concatenate(
            [outgoing[:rows]]
            + [
                exchange(outgoing[k * rows : (k + 1) * rows], "sp", k)
                for k in range(1, sp_count)
            ],
            axis=0,
        )
        pieces = [arrived]
        for bit in reversed(bits):
            pieces = pieces + [exchange(piece, "tp", bit) for piece in pieces]
        row_block = jnp.concatenate(pieces, axis=0)
        gate_act = jnp.dot(row_block, gate_weight[0], preferred_element_type=jnp.float32)
        up_act = jnp.dot(row_block, up_weight[0], preferred_element_type=jnp.float32)
        hidden = (jax.nn.silu(gate_act) * up_act).astype(jnp.bfloat16)
        partial_value = jnp.dot(
            hidden, down_weight[0], preferred_element_type=jnp.float32
        ).astype(jnp.bfloat16)
        for bit in bits:
            half = partial_value.shape[0] // 2
            received = exchange(partial_value[half:], "tp", bit)
            partial_value = (
                partial_value[:half].astype(jnp.float32) + received.astype(jnp.float32)
            ).astype(jnp.bfloat16)
        returned = jnp.concatenate(
            [partial_value[:rows]]
            + [
                exchange(partial_value[k * rows : (k + 1) * rows], "sp", k)
                for k in range(1, sp_count)
            ],
            axis=0,
        )
        high = lax.reduce_precision(weight, 8, 7).astype(jnp.bfloat16)
        low = (weight - high.astype(jnp.float32)).astype(jnp.bfloat16)
        scaled = jnp.dot(high, returned, preferred_element_type=jnp.float32) + jnp.dot(
            low, returned, preferred_element_type=jnp.float32
        )
        routed = scaled if routed is None else routed + scaled
    return (stream + routed).astype(jnp.bfloat16)


def solution(mesh):
    return jax.shard_map(
        shards,
        mesh=mesh,
        in_specs=(
            P("sp", "tp"),
            P("sp", "tp"),
            P("sp", "tp"),
            P("sp", "tp"),
            P(("sp", "tp"), None),
            P(),
            P(),
            P(("sp", "tp"), None),
            P(("sp", "tp"), None),
            P("sp", None, "tp"),
            P("sp", None, "tp"),
            P("sp", "tp", None),
        ),
        out_specs=P(("sp", "tp"), None),
        check_vma=False,
    )
```

```python
import functools

import jax
import jax.numpy as jnp
from jax import lax
from jax.experimental import pallas as pl
from jax.experimental.pallas import tpu as pltpu
from jax.sharding import PartitionSpec as P


HEAD_DIM = 64
TOP = 2
BLOCK = 256
LANES = 128
TILE = 512

epsilon = 1e-06


def exchange(value, axis, bit):
    return lax.ppermute(value, axis, [(i, i ^ bit) for i in range(lax.axis_size(axis))])


def split_of(sp_count):
    inner = 1
    while sp_count % (inner * 2) == 0 and (inner * 2) ** 2 <= sp_count:
        inner *= 2
    return sp_count // inner, inner


def one_block(query, key, value, biases, later_ones, acc, carry, mask):
    rows = query.shape[0] // len(biases)
    scores = lax.dot_general(
        query, key, (((1,), (1,)), ((), ())), preferred_element_type=jnp.float32
    )
    scores = jnp.concatenate(
        [scores[h * rows : (h + 1) * rows] + bias for h, bias in enumerate(biases)], axis=0
    )
    failure = jnp.minimum(-scores, 0.0) - jnp.log(1.0 + jnp.exp(-jnp.abs(scores)))
    if mask is not None:
        failure = jnp.where(mask, failure, 0.0)
    high = failure.astype(jnp.bfloat16)
    low = (failure - high.astype(jnp.float32)).astype(jnp.bfloat16)
    later = jnp.dot(
        jnp.concatenate([high, low], axis=0), later_ones, preferred_element_type=jnp.float32
    )
    later = later[: query.shape[0]] + later[query.shape[0] :]
    weights = jnp.exp((scores + failure) + (later + carry))
    if mask is not None:
        weights = jnp.where(mask, weights, 0.0)
    acc = acc + jnp.dot(weights.astype(jnp.bfloat16), value, preferred_element_type=jnp.float32)
    return acc, carry + later[:, :1] + failure[:, :1]


def head_queries(q_ref, heads):
    query = q_ref[...] * jnp.bfloat16(HEAD_DIM**-0.5)
    if heads == 1:
        return query
    lane_head = lax.broadcasted_iota(jnp.int32, query.shape, 1) // HEAD_DIM
    return jnp.concatenate(
        [jnp.where(lane_head == h, query, jnp.zeros_like(query)) for h in range(heads)], axis=0
    )


def later_matrix():
    row = lax.broadcasted_iota(jnp.int32, (BLOCK, BLOCK), 0)
    col = lax.broadcasted_iota(jnp.int32, (BLOCK, BLOCK), 1)
    return (row > col).astype(jnp.float32).astype(jnp.bfloat16)


def store_state(state, acc_ref, carry_ref):
    acc, carry = state
    acc_ref[...] = acc.reshape(acc_ref.shape)
    carry_ref[...] = jnp.broadcast_to(carry, (carry.shape[0], LANES)).reshape(carry_ref.shape)


def own_kernel(q_ref, kv_ref, bias_ref, acc_ref, carry_ref, *, heads, shard_len):
    tile = pl.program_id(0)
    rows, width = q_ref.shape
    query = head_queries(q_ref, heads)
    later_ones = later_matrix()
    row = tile * rows + lax.broadcasted_iota(jnp.int32, (heads * rows, BLOCK), 0) % rows
    col = lax.broadcasted_iota(jnp.int32, (heads * rows, BLOCK), 1)
    blocks = rows // BLOCK

    def step(i, state):
        block = (tile + 1) * blocks - 1 - i
        return one_block(
            query,
            kv_ref[pl.ds(block * BLOCK, BLOCK), :],
            kv_ref[pl.ds(shard_len + block * BLOCK, BLOCK), :],
            [bias_ref[block, pl.ds(h, 1), :] for h in range(heads)],
            later_ones,
            *state,
            block * BLOCK + col < row,
        )

    state = (jnp.zeros((heads * rows, width), jnp.float32), jnp.zeros((heads * rows, 1), jnp.float32))
    state = lax.fori_loop(0, (tile + 1) * blocks, step, state)
    store_state(state, acc_ref, carry_ref)


def past_kernel(
    place_ref, q_ref, kv_ref, bias_ref, acc_in, carry_in, acc_ref, carry_ref, *, heads, shard_len, inner
):
    newest, count, first, me = place_ref[0], place_ref[1], place_ref[2], place_ref[3]
    rows, width = q_ref.shape
    query = head_queries(q_ref, heads)
    later_ones = later_matrix()
    blocks = shard_len // BLOCK
    unroll = 2 if blocks % 2 == 0 else 1

    def step(i, state):
        for u in range(unroll):
            at = i * unroll + u
            piece = newest - at // blocks
            block = blocks - 1 - at % blocks
            slot = (me // inner - piece // inner - first) * inner + (
                (piece % inner) ^ (me % inner)
            )
            state = one_block(
                query,
                kv_ref[slot, pl.ds(block * BLOCK, BLOCK), :],
                kv_ref[slot, pl.ds(shard_len + block * BLOCK, BLOCK), :],
                [bias_ref[slot, block, pl.ds(h, 1), :] for h in range(heads)],
                later_ones,
                *state,
                None,
            )
        return state

    state = (
        acc_in[...].reshape(heads * rows, width),
        carry_in[...].reshape(heads * rows, LANES)[:, :1],
    )
    state = lax.fori_loop(0, count * blocks // unroll, step, state)
    store_state(state, acc_ref, carry_ref)


def attend(queries, keys, values, key_bias):
    shard_len, width = queries.shape
    heads = key_bias.shape[1]
    sp_count = lax.axis_size("sp")
    outer, inner = split_of(sp_count)
    me = lax.axis_index("sp")
    blocks = shard_len // BLOCK
    tile_rows = max(BLOCK, min(shard_len, 2 * TILE // max(heads, 2)))
    tiles = shard_len // tile_rows

    bias_rows = jnp.transpose(key_bias.reshape(blocks, BLOCK, heads), (0, 2, 1)).reshape(-1, width)
    pad = -bias_rows.shape[0] % 16
    bias_count = bias_rows.shape[0]
    own = jnp.concatenate([keys, values, jnp.pad(bias_rows, ((0, pad), (0, 0)))], axis=0)

    def bias_of(pieces):
        rows = pieces[..., 2 * shard_len : 2 * shard_len + bias_count, :]
        return rows.reshape(rows.shape[:-2] + (blocks, heads, BLOCK)).astype(jnp.float32)

    columns = [own]
    for _ in range(1, outer):
        columns.append(
            lax.ppermute(
                columns[-1],
                "sp",
                [(i, i + inner) for i in range(sp_count - inner)],
            )
        )
    groups = []
    for d in range(outer):
        groups.append([columns[d]] + [exchange(columns[d], "sp", k) for k in range(1, inner)])

    row_spec = pl.BlockSpec((tile_rows, width), lambda i: (i, 0))
    acc_spec = pl.BlockSpec((heads, tile_rows, width), lambda i: (0, i, 0))
    carry_spec = pl.BlockSpec((heads, tile_rows, LANES), lambda i: (0, i, 0))
    state_shape = (
        jax.ShapeDtypeStruct((heads, shard_len, width), jnp.float32),
        jax.ShapeDtypeStruct((heads, shard_len, LANES), jnp.float32),
    )
    whole = pl.BlockSpec(memory_space=pltpu.VMEM)
    state = pl.pallas_call(
        functools.partial(own_kernel, heads=heads, shard_len=shard_len),
        grid=(tiles,),
        in_specs=[row_spec, whole, whole],
        out_specs=(acc_spec, carry_spec),
        out_shape=state_shape,
        name="own_span",
    )(queries, own, bias_of(own))

    calls = [(0, min(2, outer))] + [(d, d + 1) for d in range(2, outer)]
    for first, end in calls:
        held = jnp.stack([piece for group in groups[first:end] for piece in group])
        newest = jnp.minimum(me - 1, (me // inner - first) * inner + inner - 1)
        oldest = jnp.maximum(0, (me // inner - end + 1) * inner)
        place = jnp.stack(
            [newest, jnp.maximum(newest - oldest + 1, 0), jnp.int32(first), me]
        ).astype(jnp.int32)
        state = pl.pallas_call(
            functools.partial(past_kernel, heads=heads, shard_len=shard_len, inner=inner),
            grid=(tiles,),
            in_specs=[
                pl.BlockSpec(memory_space=pltpu.SMEM),
                row_spec,
                whole,
                whole,
                acc_spec,
                carry_spec,
            ],
            out_specs=(acc_spec, carry_spec),
            out_shape=state_shape,
        )(place, queries, held, bias_of(held), *state)
    acc = state[0]
    lane_head = lax.iota(jnp.int32, width)[None, :] // HEAD_DIM
    attended = acc[0]
    for h in range(1, heads):
        attended = jnp.where(lane_head == h, acc[h], attended)
    return attended.astype(jnp.bfloat16)


def shards(
    queries,
    keys,
    values,
    key_bias,
    residual,
    out_weight,
    norm_gain,
    routes,
    route_weights,
    gate_weight,
    up_weight,
    down_weight,
):
    sp_count = lax.axis_size("sp")
    tp_count = lax.axis_size("tp")
    me = lax.axis_index("sp")
    attended = attend(queries, keys, values, key_bias)
    token_heads = lax.all_to_all(attended, "tp", split_axis=0, concat_axis=1, tiled=True)
    projected = jnp.dot(token_heads, out_weight, preferred_element_type=jnp.float32)
    stream = (residual.astype(jnp.float32) + projected).astype(jnp.bfloat16).astype(jnp.float32)
    normed = (
        stream * lax.rsqrt(jnp.mean(stream * stream, axis=-1, keepdims=True) + epsilon) * norm_gain
    ).astype(jnp.bfloat16)
    token_count = residual.shape[0]
    capacity = max(2, 5 * token_count * TOP // (4 * sp_count))
    flat_routes = routes.reshape(-1)
    onehot = (flat_routes[:, None] == lax.iota(jnp.int32, sp_count)[None, :]).astype(jnp.int32)
    before = jnp.cumsum(onehot, axis=0) - onehot
    position = jnp.sum(before * onehot, axis=1).reshape(token_count, TOP)
    place = routes ^ me

    first = min(capacity, -(-capacity // 16) * 8)
    chunks = [(0, first)] + ([(first, capacity)] if first < capacity else [])

    bits = []
    bit = 1
    while bit < tp_count:
        bits.append(bit)
        bit *= 2

    sent = []
    combine = []
    for begin, end in chunks:
        rows = end - begin
        inside = (position >= begin) & (position < end)
        slot = jnp.where(inside, place * rows + position - begin, -1)
        select = slot[:, :, None] == lax.iota(jnp.int32, sp_count * rows)[None, None, :]
        placing = jnp.any(select, axis=1).astype(jnp.bfloat16)
        combine.append(jnp.sum(jnp.where(select, route_weights[:, :, None], 0.0), axis=1))
        outgoing = jnp.einsum(
            "ts,td->sd", placing, normed, preferred_element_type=jnp.float32
        ).astype(jnp.bfloat16)
        sent.append(outgoing)

    routed = None
    for (begin, end), outgoing, weight in zip(chunks, sent, combine):
        rows = end - begin
        arrived = [outgoing[:rows]] + [
            exchange(outgoing[k * rows : (k + 1) * rows], "sp", k) for k in range(1, sp_count)
        ]
        pieces = [jnp.concatenate(arrived, axis=0)]
        for bit in reversed(bits):
            pieces = pieces + [exchange(piece, "tp", bit) for piece in pieces]
        row_block = jnp.concatenate(pieces, axis=0)
        gate_act = jnp.dot(row_block, gate_weight[0], preferred_element_type=jnp.float32)
        up_act = jnp.dot(row_block, up_weight[0], preferred_element_type=jnp.float32)
        hidden = (jax.nn.silu(gate_act) * up_act).astype(jnp.bfloat16)
        partial_value = jnp.dot(
            hidden, down_weight[0], preferred_element_type=jnp.float32
        ).astype(jnp.bfloat16)
        for bit in bits:
            half = partial_value.shape[0] // 2
            received = exchange(partial_value[half:], "tp", bit)
            partial_value = (
                partial_value[:half].astype(jnp.float32) + received.astype(jnp.float32)
            ).astype(jnp.bfloat16)
        returned = jnp.concatenate(
            [partial_value[:rows]]
            + [
                exchange(partial_value[k * rows : (k + 1) * rows], "sp", k)
                for k in range(1, sp_count)
            ],
            axis=0,
        )
        high = lax.reduce_precision(weight, 8, 7).astype(jnp.bfloat16)
        low = (weight - high.astype(jnp.float32)).astype(jnp.bfloat16)
        scaled = jnp.dot(high, returned, preferred_element_type=jnp.float32) + jnp.dot(
            low, returned, preferred_element_type=jnp.float32
        )
        routed = scaled if routed is None else routed + scaled
    return (stream + routed).astype(jnp.bfloat16)


def solution(mesh):
    return jax.shard_map(
        shards,
        mesh=mesh,
        in_specs=(
            P("sp", "tp"),
            P("sp", "tp"),
            P("sp", "tp"),
            P("sp", "tp"),
            P(("sp", "tp"), None),
            P(),
            P(),
            P(("sp", "tp"), None),
            P(("sp", "tp"), None),
            P("sp", None, "tp"),
            P("sp", None, "tp"),
            P("sp", "tp", None),
        ),
        out_specs=P(("sp", "tp"), None),
        check_vma=False,
    )
```
